256 devices in a mesh: kv: 16 (over y, x), tp: 16 (over z, core).
Axes of the slice: x: 4, y: 4, z: 8, core: 2. Of those that a mesh axis runs over, the one named last changes fastest.
Arguments:
- tokens: bfloat16 [1024, 4096], P(None, ('kv', 'tp')), may hold values from -10 to 10
- past_state: float32 [1024, 32, 64, 128], P('kv', 'tp'), may hold values from -6 to 6
- first_gain: float32 [4096], P('kv'), may hold values from 0.1 to 1.9
- first_gate: bfloat16 [4096, 11264], P('kv', 'tp'), may hold values from -0.09375 to 0.09375
- first_up: bfloat16 [4096, 11264], P('kv', 'tp'), may hold values from -0.09375 to 0.09375
- first_down: bfloat16 [11264, 4096], P('tp', 'kv'), may hold values from -0.078125 to 0.078125
- mix_gain: float32 [4096], P('kv'), may hold values from 0.1 to 1.9
- query_weight: bfloat16 [4096, 2048], P('kv', 'tp'), may hold values from -0.09375 to 0.09375
- key_weight: bfloat16 [4096, 2048], P('kv', 'tp'), may hold values from -0.09375 to 0.09375
- value_weight: bfloat16 [4096, 4096], P('kv', 'tp'), may hold values from -0.09375 to 0.09375
- output_gate_weight: bfloat16 [4096, 4096], P('kv', 'tp'), may hold values from -0.09375 to 0.09375
- head_gain: float32 [4096], P('tp'), may hold values from 0.1 to 1.9
- out_weight: bfloat16 [4096, 4096], P('tp', 'kv'), may hold values from -0.125 to 0.125
- second_gain: float32 [4096], P('kv'), may hold values from 0.1 to 1.9
- second_gate: bfloat16 [4096, 11264], P('kv', 'tp'), may hold values from -0.09375 to 0.09375
- second_up: bfloat16 [4096, 11264], P('kv', 'tp'), may hold values from -0.09375 to 0.09375
- second_down: bfloat16 [11264, 4096], P('tp', 'kv'), may hold values from -0.078125 to 0.078125
Outputs:
- mixed: bfloat16 [1024, 4096], P(None, ('kv', 'tp'))
- new_state: float32 [1024, 32, 64, 128], P('kv', 'tp')
The draws below stay inside these ranges and needn't reach their ends.
All inputs are finite; a program needn't handle non-finite values.
Results may differ from the reference program's by a relative error of at most 0.033.
Values may be sent and summed in bfloat16 or wider, within the bound.
No kernel may reach another device: no remote copies, remote signals or barrier semaphores. Data moves between devices by JAX's collectives and lax.ppermute only.
A program may use at most 64 MiB of HBM per device.

```python
import jax
import jax.numpy as jnp
from jax import lax

D = 4096
HEADS = 32
HEAD_K = 64
HEAD_V = 128
FF = 11264
POS = 16384
BATCH = 1024
XCOLS = 16


def draw_tokens(key, part):
    key_values, key_scales, key_common = jax.random.split(key, 3)
    block_count = D // XCOLS
    block_scale = jnp.exp(jax.random.uniform(key_scales, (block_count,), jnp.float32, jnp.log(0.35), jnp.log(2.0)))
    column_scale = jnp.repeat(block_scale, XCOLS)
    values = jnp.clip(jax.random.normal(key_values, (BATCH, D), jnp.float32), -5.0, 5.0)
    return (values * column_scale[None, :]).astype(jnp.bfloat16)


def spiked(values, stream_key, source, target, blocks, factor):
    def block_of(position):
        return (jnp.arange(values.shape[position]) // (values.shape[position] // blocks)).reshape((-1,) + (1,) * (values.ndim - 1 - position))

    one_side = jax.random.permutation(stream_key, blocks)[block_of(target)]
    other_side = (block_of(target) + blocks // 2) % blocks
    return jnp.where((block_of(source) == one_side) | (block_of(source) == other_side), factor * values, values)


def block_levels(rng, extent, shards, least, largest):
    level, own = 1.0, jax.random.fold_in(rng, 6)
    for axis_at, shards_of in shards:
        heights = jnp.exp(jax.random.uniform(jax.random.fold_in(own, axis_at), (shards_of,), jnp.float32, least / len(shards), largest / len(shards)))
        level = level * jnp.repeat(heights, extent[axis_at] // shards_of).reshape([-1 if axis == axis_at else 1 for axis in range(len(extent))])
    return level


def noise(rng, extent, scale, reach, cuts=(), kind=jnp.bfloat16):
    loudness = block_levels(rng, extent, cuts, -0.22, 0.18) if cuts else 1.0
    array = jax.random.normal(rng, extent, jnp.float32) * scale * loudness
    return jnp.minimum(jnp.maximum(array, -reach), reach).astype(kind)


def bell_draw_with(rng, dims, scale, reach, shards, heavy, kind=jnp.bfloat16):
    drawn = scale * jax.random.normal(rng, dims, jnp.float32)
    if shards:
        drawn = drawn * block_levels(rng, dims, shards, -0.22, 0.18)
    return jnp.clip(spiked(drawn, jax.random.fold_in(rng, 3), *heavy), -reach, reach).astype(kind)


def setup_inputs(seed: int = 0) -> dict:
    streams_of = jax.random.split(jax.random.key(seed), 18)
    tokens = draw_tokens(jax.random.fold_in(streams_of[17], 71), 0)
    past_state = noise(streams_of[1], (BATCH, HEADS, HEAD_K, HEAD_V), 1.0, 6.0, ((0, 16), (1, 16)), jnp.float32)
    first_gain = jnp.clip(1.0 + 0.18 * jax.random.normal(streams_of[2], (D,), jnp.float32), 0.1, 1.9)
    first_gate = noise(streams_of[3], (D, FF), D ** -0.5, 0.09375, ((0, 16), (1, 16)))
    first_up = noise(streams_of[4], (D, FF), D ** -0.5, 0.09375, ((0, 16), (1, 16)))
    first_down = bell_draw_with(streams_of[5], (FF, D), FF ** -0.5, 0.078125, ((0, 16), (1, 16)), (0, 1, 16, 2.0))
    mix_gain = jnp.clip(1.0 + 0.18 * jax.random.normal(streams_of[6], (D,), jnp.float32), 0.1, 1.9)
    query_weight = noise(streams_of[7], (D, HEADS * HEAD_K), D ** -0.5, 0.09375, ((0, 16), (1, 16)))
    key_weight = noise(streams_of[8], (D, HEADS * HEAD_K), D ** -0.5, 0.09375, ((0, 16), (1, 16)))
    value_weight = noise(streams_of[9], (D, HEADS * HEAD_V), D ** -0.5, 0.09375, ((0, 16), (1, 16)))
    output_gate_weight = noise(streams_of[10], (D, HEADS * HEAD_V), D ** -0.5, 0.09375, ((0, 16), (1, 16)))
    head_gain = jnp.clip(1.0 + 0.18 * jax.random.normal(streams_of[11], (HEADS * HEAD_V,), jnp.float32), 0.1, 1.9)
    out_weight = bell_draw_with(streams_of[12], (HEADS * HEAD_V, D), (HEADS * HEAD_V) ** -0.5, 0.125, ((0, 16), (1, 16)), (0, 1, 16, 2.0))
    second_gain = jnp.clip(1.0 + 0.18 * jax.random.normal(streams_of[13], (D,), jnp.float32), 0.1, 1.9)
    second_gate = noise(streams_of[14], (D, FF), D ** -0.5, 0.09375, ((0, 16), (1, 16)))
    second_up = noise(streams_of[15], (D, FF), D ** -0.5, 0.09375, ((0, 16), (1, 16)))
    second_down = bell_draw_with(streams_of[16], (FF, D), FF ** -0.5, 0.078125, ((0, 16), (1, 16)), (0, 1, 16, 2.0))
    return {"tokens": tokens, "past_state": past_state, "first_gain": first_gain, "first_gate": first_gate, "first_up": first_up, "first_down": first_down, "mix_gain": mix_gain, "query_weight": query_weight, "key_weight": key_weight, "value_weight": value_weight, "output_gate_weight": output_gate_weight, "head_gain": head_gain, "out_weight": out_weight, "second_gain": second_gain, "second_gate": second_gate, "second_up": second_up, "second_down": second_down}


EPS_RMS = 1e-06
EPS_GROUP = 1e-05
ROPE_BASE = 10000.0

def rotate(vectors):
    half_width = vectors.shape[-1] // 2
    frequency = ROPE_BASE ** (-jnp.arange(half_width, dtype=jnp.float32) / half_width)
    angles = POS * frequency
    cosine = jnp.cos(angles)
    sine_part = jnp.sin(angles)
    lower = vectors[..., :half_width]
    upper = vectors[..., half_width:]
    return jnp.concatenate([lower * cosine - upper * sine_part, lower * sine_part + upper * cosine], axis=-1)

def row_factor(resid_f):
    return lax.rsqrt(lax.optimization_barrier(jnp.sum(resid_f * resid_f, axis=1)) / D + EPS_RMS)[:, None]

def channel_mix(resid, gain, w_gate, w_up, w_down):
    resid_f = resid.astype(jnp.float32)
    inverse_rms = row_factor(resid_f)
    scaled = (resid_f * gain).astype(jnp.bfloat16)
    gate_sum = jnp.dot(scaled, w_gate, preferred_element_type=jnp.float32) * inverse_rms
    up_sum = jnp.dot(scaled, w_up, preferred_element_type=jnp.float32) * inverse_rms
    hidden = (jax.nn.silu(gate_sum) * up_sum).astype(jnp.bfloat16)
    branch = jnp.dot(hidden, w_down, preferred_element_type=jnp.float32)
    return (resid_f + 0.5 * branch).astype(jnp.bfloat16)

def token_mix(resid, past_state, gain, query_weight, key_weight, value_weight, output_gate_weight, head_gain, out_weight):
    resid_f = resid.astype(jnp.float32)
    row_total = resid.shape[0]
    inverse_rms = row_factor(resid_f)
    scaled = (resid_f * gain).astype(jnp.bfloat16)
    queries = jnp.dot(scaled, query_weight, preferred_element_type=jnp.float32) * inverse_rms
    keys_now = jnp.dot(scaled, key_weight, preferred_element_type=jnp.float32) * inverse_rms
    values_now = jnp.dot(scaled, value_weight, preferred_element_type=jnp.float32) * inverse_rms
    gate_now = jnp.dot(scaled, output_gate_weight, preferred_element_type=jnp.float32) * inverse_rms
    queries = rotate(queries.reshape(row_total, HEADS, HEAD_K)) * HEAD_K ** (-0.5)
    keys_now = rotate(keys_now.reshape(row_total, HEADS, HEAD_K))
    values_now = values_now.reshape(row_total, HEADS, HEAD_V)
    head_level = jnp.arange(HEADS, dtype=jnp.float32)
    retained = 1.0 - jnp.exp2(-5.0 - 16.0 * head_level / (HEADS - 1))
    new_state = retained[None, :, None, None] * past_state + keys_now[:, :, :, None] * values_now[:, :, None, :]
    retrieved = jnp.einsum('bhk,bhkv->bhv', queries, new_state, precision=lax.Precision.HIGHEST)
    head_mean = lax.optimization_barrier(jnp.mean(retrieved, axis=-1, keepdims=True))
    variance = lax.optimization_barrier(jnp.mean(jnp.square(retrieved - head_mean), axis=-1, keepdims=True))
    normed = ((retrieved - head_mean) * lax.rsqrt(variance + EPS_GROUP)).reshape(row_total, HEADS * HEAD_V) * head_gain
    mixed_heads = (jax.nn.silu(gate_now) * normed).astype(jnp.bfloat16)
    branch = jnp.dot(mixed_heads, out_weight, preferred_element_type=jnp.float32)
    return ((resid_f + branch).astype(jnp.bfloat16), new_state)

def reference(tokens, past_state, first_gain, first_gate, first_up, first_down, mix_gain, query_weight, key_weight, value_weight, output_gate_weight, head_gain, out_weight, second_gain, second_gate, second_up, second_down):
    first = channel_mix(tokens, first_gain, first_gate, first_up, first_down)
    second, new_state = token_mix(first, past_state, mix_gain, query_weight, key_weight, value_weight, output_gate_weight, head_gain, out_weight)
    mixed = channel_mix(second, second_gain, second_gate, second_up, second_down)
    return (mixed, new_state)
```

```python
import jax
import jax.numpy as jnp
from jax import lax
from jax.sharding import Mesh
from jax.sharding import PartitionSpec as P

D = 4096
HEADS = 32
HEAD_K = 64
HEAD_V = 128
POS = 16384
EPS_RMS = 1e-06
EPS_GROUP = 1e-05
ROPE_BASE = 10000.0
NY, NX, NZ, NC = 4, 4, 8, 2
LANES = 128


f32 = jnp.float32
bf16 = jnp.bfloat16


def shifted(value, axis, distance):
    size = lax.axis_size(axis)
    return lax.ppermute(value, axis, [(i, (i + distance) % size) for i in range(size)])


def exchanged(parts, axis):
    return lax.all_to_all(parts, axis, split_axis=0, concat_axis=0, tiled=True)


def for_each(value, axis):
    return exchanged(jnp.broadcast_to(value, (lax.axis_size(axis), *value.shape)), axis)


def along_x(block):
    one, three, two = (shifted(block, "x", d) for d in (1, 3, 2))
    return [block, one, two, three]


def dot(a, b):
    return jnp.dot(a, b, preferred_element_type=f32)


def rotate(vectors):
    half_width = vectors.shape[-1] // 2
    frequency = ROPE_BASE ** (-jnp.arange(half_width, dtype=f32) / half_width)
    angles = POS * frequency
    cosine = jnp.cos(angles)
    sine_part = jnp.sin(angles)
    lower = vectors[..., :half_width]
    upper = vectors[..., half_width:]
    return jnp.concatenate(
        [lower * cosine - upper * sine_part, lower * sine_part + upper * cosine], axis=-1
    )


def project(x, weights):
    width = x.shape[1] // NX
    product = sum(dot(x[:, d * width : (d + 1) * width], w) for d, w in enumerate(weights))
    x_f = x.astype(f32)
    squares = jnp.sum(x_f * x_f, axis=1, keepdims=True)
    both = jnp.concatenate(
        [product.astype(bf16), jnp.broadcast_to(squares, (x.shape[0], LANES)).astype(bf16)], axis=1
    )
    arrived = exchanged(both.reshape(NY, x.shape[0] // NY, both.shape[1]), "y").astype(f32)
    whole = arrived.sum(axis=0)
    count = product.shape[1]
    inverse_rms = lax.rsqrt(whole[:, count : count + 1] / D + EPS_RMS)
    return whole[:, :count], inverse_rms


def branch_half(inner, weights, scale):
    parts = for_each(inner, "y").reshape(NY, 2, -1, inner.shape[1])
    rows = NY * parts.shape[2]
    mine = parts[:, 0].reshape(rows, -1)
    other = parts[:, 1].reshape(rows, -1)

    def product(v):
        return jnp.concatenate([dot(v, w) for w in weights], axis=1) * scale

    arrived = shifted(product(other).astype(bf16), "c", 1)
    return (product(mine) + arrived.astype(f32)).astype(bf16)


def both_halves(mine):
    other = shifted(mine, "c", 1)
    width = mine.shape[1]
    return jnp.stack(
        [mine.reshape(NY, -1, width), other.reshape(NY, -1, width)], axis=1
    ).reshape(-1, width)


def summed_along_z(branch, residual):
    arrived = exchanged(jnp.moveaxis(branch, 1, 0), "z").astype(f32)
    return (arrived.sum(axis=0) + residual.astype(f32)).astype(bf16)


def next_input(branch, mine):
    rows = mine.shape[0]
    at = lax.axis_index("z") * LANES
    own = lax.dynamic_slice(mine, (0, at), (rows, LANES))
    piece = summed_along_z(branch.reshape(rows, NZ, LANES), own)
    return jnp.moveaxis(for_each(piece, "z"), 0, 1).reshape(rows, NZ * LANES)


def channel_inner(x, weights):
    whole, inverse_rms = project(x, weights)
    width = whole.shape[1] // 2
    gate = whole[:, :width] * inverse_rms
    up = whole[:, width:] * inverse_rms
    return (jax.nn.silu(gate) * up).astype(bf16)


def in_order(rows):
    count = rows.shape[0] // 2
    return jnp.where(
        lax.axis_index("c") == 0, rows, jnp.concatenate([rows[count:], rows[:count]], axis=0)
    )


def token_inner(x, weights, past_state, head_gain):
    whole, inverse_rms = project(x, weights)
    whole = in_order(whole * inverse_rms)
    rows, heads = past_state.shape[:2]
    keys_wide = heads * HEAD_K
    values_wide = heads * HEAD_V
    queries = whole[:, :keys_wide].reshape(rows, heads, HEAD_K)
    keys_now = whole[:, keys_wide : 2 * keys_wide].reshape(rows, heads, HEAD_K)
    values_now = whole[:, 2 * keys_wide : 2 * keys_wide + values_wide].reshape(rows, heads, HEAD_V)
    gate_now = whole[:, 2 * keys_wide + values_wide :]
    queries = rotate(queries) * HEAD_K ** (-0.5)
    keys_now = rotate(keys_now)
    first_head = (lax.axis_index("z") * NC + lax.axis_index("c")) * heads
    head_level = (first_head + jnp.arange(heads)).astype(f32)
    retained = 1.0 - jnp.exp2(-5.0 - 16.0 * head_level / (HEADS - 1))
    new_state = (
        retained[None, :, None, None] * past_state
        + keys_now[:, :, :, None] * values_now[:, :, None, :]
    )
    retrieved = jnp.einsum("bhk,bhkv->bhv", queries, new_state)
    head_mean = jnp.mean(retrieved, axis=-1, keepdims=True)
    variance = jnp.mean(jnp.square(retrieved - head_mean), axis=-1, keepdims=True)
    normed = ((retrieved - head_mean) * lax.rsqrt(variance + EPS_GROUP)).reshape(rows, values_wide)
    mixed_heads = (jax.nn.silu(gate_now) * (normed * head_gain)).astype(bf16)
    return in_order(mixed_heads), new_state


def gained(gain, *weights):
    both = jnp.concatenate(weights, axis=1).astype(f32)
    return (both * gain[:, None]).astype(bf16)


def shards(
    tokens,
    past_state,
    first_gain,
    first_gate,
    first_up,
    first_down,
    mix_gain,
    query_weight,
    key_weight,
    value_weight,
    output_gate_weight,
    head_gain,
    out_weight,
    second_gain,
    second_gate,
    second_up,
    second_down,
):
    first_in = along_x(gained(first_gain, first_gate, first_up))
    first_out = along_x(first_down)
    mix_in = along_x(gained(mix_gain, query_weight, key_weight, value_weight, output_gate_weight))
    mix_out = along_x(out_weight)
    second_in = along_x(gained(second_gain, second_gate, second_up))
    second_out = along_x(second_down)

    own_columns = tokens.shape[1]
    at_x = lax.axis_index("x")
    at_z = lax.axis_index("z")

    by_rows = tokens.reshape(NY, NX, NC, -1, own_columns)
    rows = NY * by_rows.shape[3]
    by_rows = jnp.transpose(by_rows, (1, 2, 4, 0, 3)).reshape(NX * NC, own_columns, rows)
    arrived = exchanged(by_rows, ("x", "c")).reshape(NX, NC * own_columns, rows)
    turned = jnp.concatenate([arrived[::-1], arrived[::-1]], axis=0)
    turned = lax.dynamic_slice(turned, (NX - 1 - at_x, 0, 0), arrived.shape)
    whole = for_each(turned, "z")
    mine = jnp.transpose(whole, (3, 1, 0, 2)).reshape(rows, -1)

    x = both_halves(mine)
    branch = branch_half(channel_inner(x, first_in), first_out, 0.5)
    mine = next_input(branch, mine)

    x = both_halves(mine)
    inner, state_out = token_inner(x, mix_in, past_state, head_gain)
    branch = branch_half(inner, mix_out, 1.0)
    mine = next_input(branch, mine)

    x = both_halves(mine)
    branch = branch_half(channel_inner(x, second_in), second_out, 0.5)

    piece_wide = NC * own_columns
    own = lax.dynamic_slice(
        mine.reshape(rows, NX, NZ, piece_wide), (0, 0, at_z, 0), (rows, NX, 1, piece_wide)
    ).reshape(rows, NX * piece_wide)
    ordered = jnp.transpose(branch.reshape(rows, NX, NZ, piece_wide), (0, 2, 1, 3))
    piece = summed_along_z(ordered.reshape(rows, NZ, NX * piece_wide), own)
    piece = piece.reshape(rows, NX, NC, own_columns)
    turned = jnp.transpose(piece, (1, 2, 3, 0))[::-1]
    turned = lax.dynamic_slice(
        jnp.concatenate([turned, turned], axis=0), (NX - 1 - at_x, 0, 0, 0), turned.shape
    )
    arrived = exchanged(turned.reshape(NX * NC, own_columns, rows), ("x", "c"))
    arrived = arrived.reshape(NX, NC, own_columns, NY, -1)
    mixed = jnp.transpose(arrived, (3, 0, 1, 4, 2)).reshape(tokens.shape)
    return mixed, state_out


def solution(mesh):
    chips = Mesh(mesh.devices.reshape(NY, NX, NZ, NC), ("y", "x", "z", "c"))
    kv, tp = ("y", "x"), ("z", "c")
    in_specs = (
        P(None, kv + tp),
        P(kv, tp, None, None),
        P(kv),
        P(kv, tp),
        P(kv, tp),
        P(tp, kv),
        P(kv),
        P(kv, tp),
        P(kv, tp),
        P(kv, tp),
        P(kv, tp),
        P(tp),
        P(tp, kv),
        P(kv),
        P(kv, tp),
        P(kv, tp),
        P(tp, kv),
    )
    out_specs = (P(None, kv + tp), P(kv, tp, None, None))
    return jax.shard_map(shards, mesh=chips, in_specs=in_specs, out_specs=out_specs, check_vma=False)
```

```python
import jax
import jax.numpy as jnp
from jax import lax
from jax.sharding import Mesh
from jax.sharding import PartitionSpec as P

D = 4096
HEADS = 32
HEAD_K = 64
HEAD_V = 128
POS = 16384
EPS_RMS = 1e-06
EPS_GROUP = 1e-05
ROPE_BASE = 10000.0
NY, NX, NZ, NC = 4, 4, 8, 2
LANES = 128


f32 = jnp.float32
bf16 = jnp.bfloat16


def shifted(value, axis, distance):
    size = lax.axis_size(axis)
    return lax.ppermute(value, axis, [(i, (i + distance) % size) for i in range(size)])


def exchanged(parts, axis):
    return lax.all_to_all(parts, axis, split_axis=0, concat_axis=0, tiled=True)


def for_each(value, axis):
    return exchanged(jnp.broadcast_to(value, (lax.axis_size(axis), *value.shape)), axis)


def along_x(block):
    one, three, two = (shifted(block, "x", d) for d in (1, 3, 2))
    return [block, one, two, three]


def dot(a, b):
    return jnp.dot(a, b, preferred_element_type=f32)


def rotate(vectors):
    half_width = vectors.shape[-1] // 2
    frequency = ROPE_BASE ** (-jnp.arange(half_width, dtype=f32) / half_width)
    angles = POS * frequency
    cosine = jnp.cos(angles)
    sine_part = jnp.sin(angles)
    lower = vectors[..., :half_width]
    upper = vectors[..., half_width:]
    return jnp.concatenate(
        [lower * cosine - upper * sine_part, lower * sine_part + upper * cosine], axis=-1
    )


def project(x, weights):
    width = x.shape[1] // NX
    product = sum(dot(x[:, d * width : (d + 1) * width], w) for d, w in enumerate(weights))
    x_f = x.astype(f32)
    squares = jnp.sum(x_f * x_f, axis=1, keepdims=True)
    both = jnp.concatenate(
        [product.astype(bf16), jnp.broadcast_to(squares, (x.shape[0], LANES)).astype(bf16)], axis=1
    )
    arrived = exchanged(both.reshape(NY, x.shape[0] // NY, both.shape[1]), "y").astype(f32)
    whole = arrived.sum(axis=0)
    count = product.shape[1]
    inverse_rms = lax.rsqrt(whole[:, count : count + 1] / D + EPS_RMS)
    return whole[:, :count], inverse_rms


def branch_half(inner, weights, scale):
    parts = for_each(inner, "y").reshape(NY, 2, -1, inner.shape[1])
    rows = NY * parts.shape[2]
    mine = parts[:, 0].reshape(rows, -1)
    other = parts[:, 1].reshape(rows, -1)

    def product(v):
        return jnp.concatenate([dot(v, w) for w in weights], axis=1) * scale

    arrived = shifted(product(other).astype(bf16), "c", 1)
    return (product(mine) + arrived.astype(f32)).astype(bf16)


def both_halves(mine):
    other = shifted(mine, "c", 1)
    width = mine.shape[1]
    return jnp.stack(
        [mine.reshape(NY, -1, width), other.reshape(NY, -1, width)], axis=1
    ).reshape(-1, width)


def summed_along_z(branch, residual):
    arrived = exchanged(jnp.moveaxis(branch, 1, 0), "z").astype(f32)
    return (arrived.sum(axis=0) + residual.astype(f32)).astype(bf16)


def next_input(branch, mine):
    rows = mine.shape[0]
    at = lax.axis_index("z") * LANES
    own = lax.dynamic_slice(mine, (0, at), (rows, LANES))
    piece = summed_along_z(branch.reshape(rows, NZ, LANES), own)
    return jnp.moveaxis(for_each(piece, "z"), 0, 1).reshape(rows, NZ * LANES)


def channel_inner(x, weights):
    whole, inverse_rms = project(x, weights)
    width = whole.shape[1] // 2
    gate = whole[:, :width] * inverse_rms
    up = whole[:, width:] * inverse_rms
    return (jax.nn.silu(gate) * up).astype(bf16)


def in_order(rows):
    count = rows.shape[0] // 2
    return jnp.where(
        lax.axis_index("c") == 0, rows, jnp.concatenate([rows[count:], rows[:count]], axis=0)
    )


def token_inner(x, weights, past_state, head_gain):
    whole, inverse_rms = project(x, weights)
    whole = in_order(whole * inverse_rms)
    rows, heads = past_state.shape[:2]
    keys_wide = heads * HEAD_K
    values_wide = heads * HEAD_V
    queries = whole[:, :keys_wide].reshape(rows, heads, HEAD_K)
    keys_now = whole[:, keys_wide : 2 * keys_wide].reshape(rows, heads, HEAD_K)
    values_now = whole[:, 2 * keys_wide : 2 * keys_wide + values_wide].reshape(rows, heads, HEAD_V)
    gate_now = whole[:, 2 * keys_wide + values_wide :]
    queries = rotate(queries) * HEAD_K ** (-0.5)
    keys_now = rotate(keys_now)
    first_head = (lax.axis_index("z") * NC + lax.axis_index("c")) * heads
    head_level = (first_head + jnp.arange(heads)).astype(f32)
    retained = 1.0 - jnp.exp2(-5.0 - 16.0 * head_level / (HEADS - 1))
    new_state = (
        retained[None, :, None, None] * past_state
        + keys_now[:, :, :, None] * values_now[:, :, None, :]
    )
    retrieved = jnp.einsum("bhk,bhkv->bhv", queries, new_state)
    head_mean = jnp.mean(retrieved, axis=-1, keepdims=True)
    variance = jnp.mean(jnp.square(retrieved - head_mean), axis=-1, keepdims=True)
    normed = ((retrieved - head_mean) * lax.rsqrt(variance + EPS_GROUP)).reshape(rows, values_wide)
    mixed_heads = (jax.nn.silu(gate_now) * (normed * head_gain)).astype(bf16)
    return in_order(mixed_heads), new_state


def gained(gain, *weights):
    both = jnp.concatenate(weights, axis=1).astype(f32)
    return (both * gain[:, None]).astype(bf16)


def shards(
    tokens,
    past_state,
    first_gain,
    first_gate,
    first_up,
    first_down,
    mix_gain,
    query_weight,
    key_weight,
    value_weight,
    output_gate_weight,
    head_gain,
    out_weight,
    second_gain,
    second_gate,
    second_up,
    second_down,
):
    first_in = along_x(gained(first_gain, first_gate, first_up))
    first_out = along_x(first_down)
    mix = along_x(
        jnp.concatenate(
            [
                gained(mix_gain, query_weight, key_weight),
                gained(mix_gain, value_weight),
                gained(mix_gain, output_gate_weight),
                out_weight,
            ],
            axis=0,
        ),
    )
    rows_in = query_weight.shape[0]
    mix_in = [
        jnp.concatenate([m[k * rows_in : (k + 1) * rows_in] for k in range(3)], axis=1) for m in mix
    ]
    mix_out = [m[3 * rows_in :] for m in mix]
    second_in = along_x(gained(second_gain, second_gate, second_up))
    second_out = along_x(second_down)

    own_columns = tokens.shape[1]
    at_x = lax.axis_index("x")
    at_z = lax.axis_index("z")

    by_rows = tokens.reshape(NY, NX, NC, -1, own_columns)
    rows = NY * by_rows.shape[3]
    by_rows = jnp.transpose(by_rows, (1, 2, 4, 0, 3)).reshape(NX * NC, own_columns, rows)
    arrived = exchanged(by_rows, ("x", "c")).reshape(NX, NC * own_columns, rows)
    turned = jnp.concatenate([arrived[::-1], arrived[::-1]], axis=0)
    turned = lax.dynamic_slice(turned, (NX - 1 - at_x, 0, 0), arrived.shape)
    whole = for_each(turned, "z")
    mine = jnp.transpose(whole, (3, 1, 0, 2)).reshape(rows, -1)

    x = both_halves(mine)
    branch = branch_half(channel_inner(x, first_in), first_out, 0.5)
    mine = next_input(branch, mine)

    x = both_halves(mine)
    inner, state_out = token_inner(x, mix_in, past_state, head_gain)
    branch = branch_half(inner, mix_out, 1.0)
    mine = next_input(branch, mine)

    x = both_halves(mine)
    branch = branch_half(channel_inner(x, second_in), second_out, 0.5)

    piece_wide = NC * own_columns
    own = lax.dynamic_slice(
        mine.reshape(rows, NX, NZ, piece_wide), (0, 0, at_z, 0), (rows, NX, 1, piece_wide)
    ).reshape(rows, NX * piece_wide)
    ordered = jnp.transpose(branch.reshape(rows, NX, NZ, piece_wide), (0, 2, 1, 3))
    piece = summed_along_z(ordered.reshape(rows, NZ, NX * piece_wide), own)
    piece = piece.reshape(rows, NX, NC, own_columns)
    turned = jnp.transpose(piece, (1, 2, 3, 0))[::-1]
    turned = lax.dynamic_slice(
        jnp.concatenate([turned, turned], axis=0), (NX - 1 - at_x, 0, 0, 0), turned.shape
    )
    arrived = exchanged(turned.reshape(NX * NC, own_columns, rows), ("x", "c"))
    arrived = arrived.reshape(NX, NC, own_columns, NY, -1)
    mixed = jnp.transpose(arrived, (3, 0, 1, 4, 2)).reshape(tokens.shape)
    return mixed, state_out


def solution(mesh):
    chips = Mesh(mesh.devices.reshape(NY, NX, NZ, NC), ("y", "x", "z", "c"))
    kv, tp = ("y", "x"), ("z", "c")
    in_specs = (
        P(None, kv + tp),
        P(kv, tp, None, None),
        P(kv),
        P(kv, tp),
        P(kv, tp),
        P(tp, kv),
        P(kv),
        P(kv, tp),
        P(kv, tp),
        P(kv, tp),
        P(kv, tp),
        P(tp),
        P(tp, kv),
        P(kv),
        P(kv, tp),
        P(kv, tp),
        P(tp, kv),
    )
    out_specs = (P(None, kv + tp), P(kv, tp, None, None))
    return jax.shard_map(shards, mesh=chips, in_specs=in_specs, out_specs=out_specs, check_vma=False)
```

```python
import jax
import jax.numpy as jnp
from jax import lax
from jax.sharding import Mesh
from jax.sharding import PartitionSpec as P

D = 4096
HEADS = 32
HEAD_K = 64
HEAD_V = 128
POS = 16384
EPS_RMS = 1e-06
EPS_GROUP = 1e-05
ROPE_BASE = 10000.0
NY, NX, NZ, NC = 4, 4, 8, 2
LANES = 128


f32 = jnp.float32
bf16 = jnp.bfloat16


def shifted(value, axis, distance):
    size = lax.axis_size(axis)
    return lax.ppermute(value, axis, [(i, (i + distance) % size) for i in range(size)])


def exchanged(parts, axis):
    return lax.all_to_all(parts, axis, split_axis=0, concat_axis=0, tiled=True)


def for_each(value, axis):
    return exchanged(jnp.broadcast_to(value, (lax.axis_size(axis), *value.shape)), axis)


def along_x(block):
    one, three, two = (shifted(block, "x", d) for d in (1, 3, 2))
    return [block, one, two, three]


def by_distance(parts, axis):
    count = parts.shape[0]
    turned = jnp.concatenate([parts[::-1], parts[::-1]], axis=0)
    return lax.dynamic_slice_in_dim(turned, count - 1 - lax.axis_index(axis), count, axis=0)


def dot(a, b):
    return jnp.dot(a, b, preferred_element_type=f32)


def rotate(vectors):
    half_width = vectors.shape[-1] // 2
    frequency = ROPE_BASE ** (-jnp.arange(half_width, dtype=f32) / half_width)
    angles = POS * frequency
    cosine = jnp.cos(angles)
    sine_part = jnp.sin(angles)
    lower = vectors[..., :half_width]
    upper = vectors[..., half_width:]
    return jnp.concatenate(
        [lower * cosine - upper * sine_part, lower * sine_part + upper * cosine], axis=-1
    )


def project(x, weights):
    width = x.shape[1] // NX
    product = sum(dot(x[:, d * width : (d + 1) * width], w) for d, w in enumerate(weights))
    x_f = x.astype(f32)
    squares = jnp.sum(x_f * x_f, axis=1, keepdims=True)
    both = jnp.concatenate([product, jnp.broadcast_to(squares, (x.shape[0], LANES))], axis=1)
    both = both.reshape(NY, x.shape[0] // NY, both.shape[1])
    sent = both.astype(bf16)
    arrived = [shifted(sent[d], "y", -d) for d in (1, 3, 2)]
    whole = both[0] + sum(a.astype(f32) for a in arrived)
    count = product.shape[1]
    inverse_rms = lax.rsqrt(whole[:, count : count + 1] / D + EPS_RMS)
    return whole[:, :count], inverse_rms


def branch_half(inner, weights, scale):
    one, three, two = (shifted(inner, "y", d) for d in (1, 3, 2))
    parts = [inner, one, two, three]
    count = inner.shape[0] // NC
    mine = jnp.concatenate([p[:count] for p in parts], axis=0)
    other = jnp.concatenate([p[count:] for p in parts], axis=0)

    def product(v):
        return jnp.concatenate([dot(v, w) for w in weights], axis=1) * scale

    sent = product(other).astype(bf16)
    arrived = shifted(sent, "c", 1)
    return product(mine) + arrived.astype(f32)


def both_halves(mine):
    other = shifted(mine, "c", 1)
    width = mine.shape[1]
    return jnp.stack(
        [mine.reshape(NY, -1, width), other.reshape(NY, -1, width)], axis=1
    ).reshape(-1, width)


def next_input(branch, mine):
    rows = mine.shape[0]
    own = lax.dynamic_slice(mine, (0, lax.axis_index("z") * LANES), (rows, LANES))
    parts = jnp.moveaxis(branch.astype(bf16).reshape(rows, NZ, LANES), 1, 0)
    arrived = exchanged(parts, "z").astype(f32)
    piece = (arrived.sum(axis=0) + own.astype(f32)).astype(bf16)
    return jnp.moveaxis(for_each(piece, "z"), 0, 1).reshape(rows, NZ * LANES)


def channel_inner(x, weights):
    whole, inverse_rms = project(x, weights)
    width = whole.shape[1] // 2
    gate = whole[:, :width] * inverse_rms
    up = whole[:, width:] * inverse_rms
    return (jax.nn.silu(gate) * up).astype(bf16)


def in_order(rows):
    count = rows.shape[0] // 2
    return jnp.where(
        lax.axis_index("c") == 0, rows, jnp.concatenate([rows[count:], rows[:count]], axis=0)
    )


def token_inner(x, weights, past_state, head_gain):
    whole, inverse_rms = project(x, weights)
    whole = in_order(whole * inverse_rms)
    rows, heads = past_state.shape[:2]
    keys_wide = heads * HEAD_K
    values_wide = heads * HEAD_V
    queries = whole[:, :keys_wide].reshape(rows, heads, HEAD_K)
    keys_now = whole[:, keys_wide : 2 * keys_wide].reshape(rows, heads, HEAD_K)
    values_now = whole[:, 2 * keys_wide : 2 * keys_wide + values_wide].reshape(rows, heads, HEAD_V)
    gate_now = whole[:, 2 * keys_wide + values_wide :]
    queries = rotate(queries) * HEAD_K ** (-0.5)
    keys_now = rotate(keys_now)
    first_head = (lax.axis_index("z") * NC + lax.axis_index("c")) * heads
    head_level = (first_head + jnp.arange(heads)).astype(f32)
    retained = 1.0 - jnp.exp2(-5.0 - 16.0 * head_level / (HEADS - 1))
    new_state = (
        retained[None, :, None, None] * past_state
        + keys_now[:, :, :, None] * values_now[:, :, None, :]
    )
    retrieved = jnp.einsum("bhk,bhkv->bhv", queries, new_state)
    head_mean = jnp.mean(retrieved, axis=-1, keepdims=True)
    variance = jnp.mean(jnp.square(retrieved - head_mean), axis=-1, keepdims=True)
    normed = ((retrieved - head_mean) * lax.rsqrt(variance + EPS_GROUP)).reshape(rows, values_wide)
    mixed_heads = (jax.nn.silu(gate_now) * (normed * head_gain)).astype(bf16)
    return in_order(mixed_heads), new_state


def gained(gain, *weights):
    both = jnp.concatenate(weights, axis=1).astype(f32)
    return (both * gain[:, None]).astype(bf16)


def shards(
    tokens,
    past_state,
    first_gain,
    first_gate,
    first_up,
    first_down,
    mix_gain,
    query_weight,
    key_weight,
    value_weight,
    output_gate_weight,
    head_gain,
    out_weight,
    second_gain,
    second_gate,
    second_up,
    second_down,
):
    first_in = along_x(gained(first_gain, first_gate, first_up))
    first_out = along_x(first_down)
    mix = along_x(
        jnp.concatenate(
            [
                gained(mix_gain, query_weight, key_weight),
                gained(mix_gain, value_weight),
                gained(mix_gain, output_gate_weight),
                out_weight,
            ],
            axis=0,
        ),
    )
    rows_in = query_weight.shape[0]
    mix_in = [
        jnp.concatenate([m[k * rows_in : (k + 1) * rows_in] for k in range(3)], axis=1) for m in mix
    ]
    mix_out = [m[3 * rows_in :] for m in mix]
    second_in = along_x(gained(second_gain, second_gate, second_up))
    second_out = along_x(second_down)

    own_columns = tokens.shape[1]
    sizes = (NX, NZ, NC)

    by_rows = by_distance(tokens.reshape(NY, NX, NC, -1, own_columns), "y")
    rows = NY * by_rows.shape[3]
    by_rows = jnp.transpose(by_rows, (1, 2, 4, 0, 3)).reshape(NX, 1, NC, own_columns, rows)
    by_rows = jnp.broadcast_to(by_rows, (NX, NZ, NC, own_columns, rows))
    arrived = exchanged(by_rows.reshape(-1, own_columns, rows), ("x", "z", "c"))
    mine = by_distance(arrived.reshape(NX, -1, rows), "x").reshape(-1, rows).T

    x = both_halves(mine)
    branch = branch_half(channel_inner(x, first_in), first_out, 0.5)
    mine = next_input(branch, mine)

    x = both_halves(mine)
    inner, state_out = token_inner(x, mix_in, past_state, head_gain)
    branch = branch_half(inner, mix_out, 1.0)
    mine = next_input(branch, mine)

    x = both_halves(mine)
    branch = branch_half(channel_inner(x, second_in), second_out, 0.5)

    owner = jnp.arange(NZ * LANES) // LANES == lax.axis_index("z")
    branch = (branch + jnp.where(owner[None, :], mine.astype(f32), 0.0)).astype(bf16)
    turned = by_distance(branch.T.reshape(NX, -1, rows), "x")
    arrived = exchanged(turned.reshape(-1, own_columns, rows), ("x", "z", "c"))
    arrived = arrived.reshape(*sizes, own_columns, rows).astype(f32).sum(axis=1).astype(bf16)
    arrived = arrived.reshape(NX, NC, own_columns, NY, -1)
    mixed = by_distance(jnp.transpose(arrived, (3, 0, 1, 4, 2)), "y").reshape(tokens.shape)
    return mixed, state_out


def solution(mesh):
    chips = Mesh(mesh.devices.reshape(NY, NX, NZ, NC), ("y", "x", "z", "c"))
    kv, tp = ("y", "x"), ("z", "c")
    in_specs = (
        P(None, kv + tp),
        P(kv, tp, None, None),
        P(kv),
        P(kv, tp),
        P(kv, tp),
        P(tp, kv),
        P(kv),
        P(kv, tp),
        P(kv, tp),
        P(kv, tp),
        P(kv, tp),
        P(tp),
        P(tp, kv),
        P(kv),
        P(kv, tp),
        P(kv, tp),
        P(tp, kv),
    )
    out_specs = (P(None, kv + tp), P(kv, tp, None, None))
    return jax.shard_map(shards, mesh=chips, in_specs=in_specs, out_specs=out_specs, check_vma=False)
```

```python
import jax
import jax.numpy as jnp
from jax import lax
from jax.experimental import pallas as pl
from jax.sharding import Mesh
from jax.sharding import PartitionSpec as P

D = 4096
HEADS = 32
HEAD_K = 64
HEAD_V = 128
POS = 16384
EPS_RMS = 1e-06
EPS_GROUP = 1e-05
ROPE_BASE = 10000.0
NY, NX, NZ, NC = 4, 4, 8, 2
LANES = 128


f32 = jnp.float32
bf16 = jnp.bfloat16


def shifted(value, axis, distance):
    size = lax.axis_size(axis)
    return lax.ppermute(value, axis, [(i, (i + distance) % size) for i in range(size)])


def exchanged(parts, axis):
    return lax.all_to_all(parts, axis, split_axis=0, concat_axis=0, tiled=True)


def for_each(value, axis):
    return exchanged(jnp.broadcast_to(value, (lax.axis_size(axis), *value.shape)), axis)


def along_x(block):
    one, three, two = (shifted(block, "x", d) for d in (1, 3, 2))
    return [block, one, two, three]


def by_distance(parts, axis):
    count = parts.shape[0]
    turned = jnp.concatenate([parts[::-1], parts[::-1]], axis=0)
    return lax.dynamic_slice_in_dim(turned, count - 1 - lax.axis_index(axis), count, axis=0)


def dot(a, b):
    return jnp.dot(a, b, preferred_element_type=f32)


def rotate(vectors):
    half_width = vectors.shape[-1] // 2
    frequency = ROPE_BASE ** (-jnp.arange(half_width, dtype=f32) / half_width)
    angles = POS * frequency
    cosine = jnp.cos(angles)
    sine_part = jnp.sin(angles)
    lower = vectors[..., :half_width]
    upper = vectors[..., half_width:]
    return jnp.concatenate(
        [lower * cosine - upper * sine_part, lower * sine_part + upper * cosine], axis=-1
    )


def project_body(blocks, mine, other, w0, w1, w2, w3, own, s1, s2, s3):
    weights = (w0, w1, w2, w3)
    x = jnp.concatenate(
        [jnp.concatenate([half[k] for k in range(NZ)], axis=1) for half in (mine, other)], axis=0
    )
    count = x.shape[0] // 2
    rows = count // NY

    def put(at, value):
        wide = pl.ds(at, value.shape[1])
        for h in range(2):
            for d, target in enumerate((own, s1, s2, s3)):
                part = value[h * count + d * rows : h * count + (d + 1) * rows]
                target[h * rows : (h + 1) * rows, wide] = part.astype(target.dtype)

    x_f = x.astype(f32)
    squares = jnp.sum(x_f * x_f, axis=1, keepdims=True)
    put(own.shape[1] - LANES, jnp.broadcast_to(squares, (x.shape[0], LANES)))
    width = w0.shape[0] // blocks
    start = 0
    depth = x.shape[1] // NX
    while start < own.shape[1] - LANES:
        size = min(2 * LANES, own.shape[1] - LANES - start)
        if blocks == 1:
            tiles = [w[:, start : start + size] for w in weights]
        else:
            at = start // size * width
            tiles = [w[at : at + width] for w in weights]
        put(start, sum(dot(x[:, d * depth : (d + 1) * depth], t) for d, t in enumerate(tiles)))
        start += size


def project(mine, weights, count):
    other = shifted(mine, "c", 1)
    rows = 2 * mine.shape[1] // NY
    shape = (rows, count + LANES)
    blocks = 1 if weights[0].shape[1] == count else 4
    own, *sent = pl.pallas_call(
        lambda *refs: project_body(blocks, *refs),
        out_shape=[jax.ShapeDtypeStruct(shape, t) for t in (f32, bf16, bf16, bf16)],
    )(mine, other, *weights)
    return [own] + [shifted(sent[d - 1], "y", -d) for d in (1, 3, 2)]


def branch_body(first_row, scale, p0, p1, p2, p3, w0, w1, w2, w3, mine, other):
    parts = [p[...] for p in (p0, p1, p2, p3)]
    count = p0.shape[0] // 2
    both = jnp.concatenate([p[:count] for p in parts] + [p[count:] for p in parts], axis=0)
    rows = NY * count
    for d, w in enumerate((w0, w1, w2, w3)):
        product = dot(both, w[first_row : first_row + p0.shape[1]]) * scale
        for k in range(product.shape[1] // LANES):
            piece = product[:, k * LANES : (k + 1) * LANES]
            at = d * (product.shape[1] // LANES) + k
            mine[at] = piece[:rows]
            other[at] = piece[rows:].astype(other.dtype)


def branch_half(inner, weights, first_row, scale):
    one, three, two = (shifted(inner, "y", d) for d in (1, 3, 2))
    shape = (NZ, NY * inner.shape[0] // 2, LANES)
    mine, other = pl.pallas_call(
        lambda *refs: branch_body(first_row, scale, *refs),
        out_shape=[jax.ShapeDtypeStruct(shape, f32), jax.ShapeDtypeStruct(shape, bf16)],
    )(inner, one, two, three, *weights)
    arrived = shifted(other, "c", 1)
    return mine + arrived.astype(f32)


def next_input(branch, mine):
    own = lax.dynamic_index_in_dim(mine, lax.axis_index("z"), keepdims=False)
    arrived = exchanged(branch.astype(bf16), "z").astype(f32)
    piece = (arrived.sum(axis=0) + own.astype(f32)).astype(bf16)
    return for_each(piece, "z")


def silu(v):
    return v / (1.0 + jnp.exp(-v))


def activate_body(own, a1, a2, a3, out):
    whole = own[...] + a1[...].astype(f32) + a2[...].astype(f32) + a3[...].astype(f32)
    count = whole.shape[1] - LANES
    whole = whole[:, :count] * lax.rsqrt(whole[:, count : count + 1] / D + EPS_RMS)
    even = count // (2 * LANES) * LANES
    out[:, :even] = (silu(whole[:, :even]) * whole[:, even : 2 * even]).astype(bf16)
    rest = whole[:, 2 * even :]
    half = rest.shape[1] // 2
    out[:, even:] = (silu(rest[:, :half]) * rest[:, half:]).astype(bf16)


def channel_inner(mine, weights):
    count = weights[0].shape[1]
    parts = project(mine, weights, count)
    return pl.pallas_call(
        activate_body, out_shape=jax.ShapeDtypeStruct((parts[0].shape[0], count // 2), bf16)
    )(*parts)


def in_order(rows):
    count = rows.shape[0] // 2
    return jnp.where(
        lax.axis_index("c") == 0, rows, jnp.concatenate([rows[count:], rows[:count]], axis=0)
    )


def token_inner(mine, weights, past_state, head_gain):
    rows, heads = past_state.shape[:2]
    keys_wide = heads * HEAD_K
    values_wide = heads * HEAD_V
    count = 2 * (keys_wide + values_wide)
    whole = sum(p.astype(f32) for p in project(mine, weights, count))
    inverse_rms = lax.rsqrt(whole[:, count : count + 1] / D + EPS_RMS)
    whole = in_order(whole[:, :count] * inverse_rms)
    queries = whole[:, :keys_wide].reshape(rows, heads, HEAD_K)
    keys_now = whole[:, keys_wide : 2 * keys_wide].reshape(rows, heads, HEAD_K)
    values_now = whole[:, 2 * keys_wide : 2 * keys_wide + values_wide].reshape(rows, heads, HEAD_V)
    gate_now = whole[:, 2 * keys_wide + values_wide :]
    queries = rotate(queries) * HEAD_K ** (-0.5)
    keys_now = rotate(keys_now)
    first_head = (lax.axis_index("z") * NC + lax.axis_index("c")) * heads
    head_level = (first_head + jnp.arange(heads)).astype(f32)
    retained = 1.0 - jnp.exp2(-5.0 - 16.0 * head_level / (HEADS - 1))
    new_state = (
        retained[None, :, None, None] * past_state
        + keys_now[:, :, :, None] * values_now[:, :, None, :]
    )
    retrieved = jnp.einsum("bhk,bhkv->bhv", queries, new_state)
    head_mean = jnp.mean(retrieved, axis=-1, keepdims=True)
    variance = jnp.mean(jnp.square(retrieved - head_mean), axis=-1, keepdims=True)
    normed = ((retrieved - head_mean) * lax.rsqrt(variance + EPS_GROUP)).reshape(rows, values_wide)
    mixed_heads = (jax.nn.silu(gate_now) * (normed * head_gain)).astype(bf16)
    return in_order(mixed_heads), new_state


def gained(gain, *weights):
    both = jnp.concatenate(weights, axis=1).astype(f32)
    return (both * gain[:, None]).astype(bf16)


def paired(gate, up):
    even = gate.shape[1] // LANES * LANES
    return gate[:, :even], up[:, :even], gate[:, even:], up[:, even:]


def shards(
    tokens,
    past_state,
    first_gain,
    first_gate,
    first_up,
    first_down,
    mix_gain,
    query_weight,
    key_weight,
    value_weight,
    output_gate_weight,
    head_gain,
    out_weight,
    second_gain,
    second_gate,
    second_up,
    second_down,
):
    first_in = along_x(gained(first_gain, *paired(first_gate, first_up)))
    first_out = along_x(first_down)
    mix = along_x(
        jnp.concatenate(
            [
                gained(mix_gain, query_weight, key_weight),
                gained(mix_gain, value_weight),
                gained(mix_gain, output_gate_weight),
                out_weight,
            ],
            axis=0,
        ),
    )
    second_in = along_x(gained(second_gain, *paired(second_gate, second_up)))
    second_out = along_x(second_down)

    own_columns = tokens.shape[1]
    sizes = (NX, NZ, NC)

    by_rows = by_distance(tokens.reshape(NY, NX, NC, -1, own_columns), "y")
    rows = NY * by_rows.shape[3]
    by_rows = jnp.transpose(by_rows, (1, 2, 4, 0, 3)).reshape(NX * NC, own_columns, rows)
    arrived = exchanged(by_rows, ("x", "c")).reshape(NX, NC * own_columns, rows)
    whole = for_each(by_distance(arrived, "x"), "z")
    ordered = jnp.moveaxis(whole, 1, 0).reshape(NZ, LANES, rows)
    mine = jnp.swapaxes(ordered, 1, 2)

    branch = branch_half(channel_inner(mine, first_in), first_out, 0, 0.5)
    mine = next_input(branch, mine)

    inner, state_out = token_inner(mine, mix, past_state, head_gain)
    branch = branch_half(inner, mix, 3 * query_weight.shape[0], 1.0)
    mine = next_input(branch, mine)

    branch = branch_half(channel_inner(mine, second_in), second_out, 0, 0.5)

    owner = jnp.arange(NZ) == lax.axis_index("z")
    branch = (branch + jnp.where(owner[:, None, None], mine.astype(f32), 0.0)).astype(bf16)
    turned = by_distance(jnp.swapaxes(branch, 1, 2).reshape(NX, -1, rows), "x")
    arrived = exchanged(turned.reshape(-1, own_columns, rows), ("x", "z", "c"))
    arrived = arrived.reshape(*sizes, own_columns, rows).astype(f32).sum(axis=1).astype(bf16)
    arrived = arrived.reshape(NX, NC, own_columns, NY, -1)
    mixed = by_distance(jnp.transpose(arrived, (3, 0, 1, 4, 2)), "y").reshape(tokens.shape)
    return mixed, state_out


def solution(mesh):
    chips = Mesh(mesh.devices.reshape(NY, NX, NZ, NC), ("y", "x", "z", "c"))
    kv, tp = ("y", "x"), ("z", "c")
    in_specs = (
        P(None, kv + tp),
        P(kv, tp, None, None),
        P(kv),
        P(kv, tp),
        P(kv, tp),
        P(tp, kv),
        P(kv),
        P(kv, tp),
        P(kv, tp),
        P(kv, tp),
        P(kv, tp),
        P(tp),
        P(tp, kv),
        P(kv),
        P(kv, tp),
        P(kv, tp),
        P(tp, kv),
    )
    out_specs = (P(None, kv + tp), P(kv, tp, None, None))
    return jax.shard_map(shards, mesh=chips, in_specs=in_specs, out_specs=out_specs, check_vma=False)
```

```python
import jax
import jax.numpy as jnp
from jax import lax
from jax.experimental import pallas as pl
from jax.sharding import Mesh
from jax.sharding import PartitionSpec as P

D = 4096
HEADS = 32
HEAD_K = 64
HEAD_V = 128
POS = 16384
EPS_RMS = 1e-06
EPS_GROUP = 1e-05
ROPE_BASE = 10000.0
NY, NX, NZ, NC = 4, 4, 8, 2
LANES = 128


f32 = jnp.float32
bf16 = jnp.bfloat16


def shifted(value, axis, distance):
    size = lax.axis_size(axis)
    return lax.ppermute(value, axis, [(i, (i + distance) % size) for i in range(size)])


def exchanged(parts, axis):
    return lax.all_to_all(parts, axis, split_axis=0, concat_axis=0, tiled=True)


def for_each(value, axis):
    return exchanged(jnp.broadcast_to(value, (lax.axis_size(axis), *value.shape)), axis)


def along_x(block):
    one, three, two = (shifted(block, "x", d) for d in (1, 3, 2))
    return [block, one, two, three]


def along_x_by_relay(left, right):
    left_one = shifted(left, "x", 1)
    right_three = shifted(right, "x", -1)
    right_one = shifted(right, "x", 1)
    left_three = shifted(left, "x", -1)
    left_two = shifted(left_one, "x", 1)
    right_two = shifted(right_three, "x", -1)
    return [left, left_one, left_two, left_three], [right, right_one, right_two, right_three]


def by_distance(parts, axis):
    count = parts.shape[0]
    turned = jnp.concatenate([parts[::-1], parts[::-1]], axis=0)
    return lax.dynamic_slice_in_dim(turned, count - 1 - lax.axis_index(axis), count, axis=0)


def dot(a, b):
    return jnp.dot(a, b, preferred_element_type=f32)


def rotate(vectors):
    half_width = vectors.shape[-1] // 2
    frequency = ROPE_BASE ** (-jnp.arange(half_width, dtype=f32) / half_width)
    angles = POS * frequency
    cosine = jnp.cos(angles)
    sine_part = jnp.sin(angles)
    lower = vectors[..., :half_width]
    upper = vectors[..., half_width:]
    return jnp.concatenate(
        [lower * cosine - upper * sine_part, lower * sine_part + upper * cosine], axis=-1
    )


def times(x, weights, count):
    width = x.shape[1] // NX
    return sum(
        dot(x[:, d * width : (d + 1) * width], weights[d][:, :count]) for d in (0, 1, 3, 2)
    )


def project(x, product):
    count = product.shape[1]
    x_f = x.astype(f32)
    squares = jnp.sum(x_f * x_f, axis=1, keepdims=True)
    both = jnp.concatenate([product, jnp.broadcast_to(squares, (x.shape[0], LANES))], axis=1)
    both = both.reshape(NY, x.shape[0] // NY, both.shape[1])
    sent = both.astype(bf16)
    arrived = [shifted(sent[d], "y", -d) for d in (1, 3, 2)]
    whole = both[0] + sum(a.astype(f32) for a in arrived)
    inverse_rms = lax.rsqrt(whole[:, count : count + 1] / D + EPS_RMS)
    return whole[:, :count], inverse_rms


def first_body(mine, other, *refs):
    left, right, targets = refs[:NX], refs[NX : 2 * NX], refs[2 * NX :]
    x = jnp.concatenate([mine[...], other[...]], axis=0)
    count = x.shape[0] // 2
    rows = count // NY
    depth = x.shape[1] // NX
    width = left[0].shape[1]

    def put(at, value):
        for h in range(2):
            for d, target in enumerate(targets):
                part = value[h * count + d * rows : h * count + (d + 1) * rows]
                target[h * rows : (h + 1) * rows, at : at + value.shape[1]] = part.astype(
                    target.dtype
                )

    x_f = x.astype(f32)
    squares = jnp.sum(x_f * x_f, axis=1, keepdims=True)
    for place, weights in ((0, left), (targets[0].shape[1] // 2, right)):
        for start in range(0, width, 2 * LANES):
            size = min(2 * LANES, width - start)
            product = sum(
                dot(x[:, d * depth : (d + 1) * depth], w[:, start : start + size])
                for d, w in enumerate(weights)
            )
            spare = -size % LANES
            if spare:
                fill = jnp.broadcast_to(squares, (x.shape[0], spare))
                product = jnp.concatenate([product, fill], axis=1)
            put(place + start, product)


def first_inner(mine, weights):
    other = shifted(mine, "c", 1)
    left, right = weights
    width = left[0].shape[1]
    wide = width + -width % LANES
    shape = (2 * mine.shape[0] // NY, 2 * wide)
    own, *sent = pl.pallas_call(
        first_body,
        out_shape=[jax.ShapeDtypeStruct(shape, t) for t in (f32, bf16, bf16, bf16)],
        name="first",
    )(mine, other, *left, *right)
    arrived = [shifted(sent[d - 1], "y", -d) for d in (1, 3, 2)]
    whole = own + sum(a.astype(f32) for a in arrived)
    inverse_rms = lax.rsqrt(whole[:, width : width + 1] / D + EPS_RMS)
    gate = whole[:, :width] * inverse_rms
    up = whole[:, wide : wide + width] * inverse_rms
    return (jax.nn.silu(gate) * up).astype(bf16)


def branch_body(scale, p0, p1, p2, p3, w0, w1, w2, w3, mine, other):
    parts = [p[...] for p in (p0, p1, p2, p3)]
    count = p0.shape[0] // 2
    both = jnp.concatenate([p[:count] for p in parts] + [p[count:] for p in parts], axis=0)
    rows = NY * count
    for d, w in enumerate((w0, w1, w2, w3)):
        product = dot(both, w[...]) * scale
        for k in range(product.shape[1] // LANES):
            piece = product[:, k * LANES : (k + 1) * LANES]
            at = d * (product.shape[1] // LANES) + k
            mine[at] = piece[:rows]
            other[at] = piece[rows:].astype(other.dtype)


def branch_half(inner, weights, scale):
    one, three, two = (shifted(inner, "y", d) for d in (1, 3, 2))
    parts = (inner, one, two, three)
    depth, columns = weights[0].shape
    width = NZ * LANES // NX
    shape = (NZ, NY * inner.shape[0] // 2, LANES)
    whole = pl.BlockSpec(inner.shape, lambda i: (0, 0))
    last = pl.BlockSpec((depth, width), lambda i: (0, columns // width - 1))
    out = pl.BlockSpec(shape, lambda i: (0, 0, 0))
    mine, other = pl.pallas_call(
        lambda *refs: branch_body(scale, *refs),
        grid=(1,),
        in_specs=[whole] * NY + [last] * NX,
        out_specs=[out, out],
        out_shape=[jax.ShapeDtypeStruct(shape, f32), jax.ShapeDtypeStruct(shape, bf16)],
    )(*parts, *weights)
    arrived = shifted(other, "c", 1)
    return mine + arrived.astype(f32)


def branch_half_in_turn(inner, weights, scale):
    one, three, two = (shifted(inner, "y", d) for d in (1, 3, 2))
    parts = [inner, one, two, three]
    count = inner.shape[0] // NC
    mine = jnp.concatenate([p[:count] for p in parts], axis=0)
    other = jnp.concatenate([p[count:] for p in parts], axis=0)

    def product(v):
        return jnp.concatenate([dot(v, w) for w in weights], axis=1) * scale

    sent = product(other).astype(bf16)
    arrived = shifted(sent, "c", 1)
    whole = product(mine) + arrived.astype(f32)
    return jnp.moveaxis(whole.astype(bf16).reshape(-1, NZ, LANES), 1, 0)


def both_halves(mine):
    other = shifted(mine, "c", 1)
    width = mine.shape[1]
    return jnp.stack(
        [mine.reshape(NY, -1, width), other.reshape(NY, -1, width)], axis=1
    ).reshape(-1, width)


def next_input(branch, mine):
    rows = mine.shape[0]
    own = lax.dynamic_slice(mine, (0, lax.axis_index("z") * LANES), (rows, LANES))
    arrived = exchanged(branch.astype(bf16), "z").astype(f32)
    piece = (arrived.sum(axis=0) + own.astype(f32)).astype(bf16)
    return jnp.moveaxis(for_each(piece, "z"), 0, 1).reshape(rows, NZ * LANES)


def channel_inner(x, product):
    whole, inverse_rms = project(x, product)
    width = whole.shape[1] // 2
    gate = whole[:, :width] * inverse_rms
    up = whole[:, width:] * inverse_rms
    return (jax.nn.silu(gate) * up).astype(bf16)


def in_order(rows):
    count = rows.shape[0] // 2
    return jnp.where(
        lax.axis_index("c") == 0, rows, jnp.concatenate([rows[count:], rows[:count]], axis=0)
    )


def token_inner(x, weights, past_state, head_gain):
    rows, heads = past_state.shape[:2]
    keys_wide = heads * HEAD_K
    values_wide = heads * HEAD_V
    whole, inverse_rms = project(x, times(x, weights, 2 * (keys_wide + values_wide)))
    whole = in_order(whole * inverse_rms)
    queries = whole[:, :keys_wide].reshape(rows, heads, HEAD_K)
    keys_now = whole[:, keys_wide : 2 * keys_wide].reshape(rows, heads, HEAD_K)
    values_now = whole[:, 2 * keys_wide : 2 * keys_wide + values_wide].reshape(rows, heads, HEAD_V)
    gate_now = whole[:, 2 * keys_wide + values_wide :]
    queries = rotate(queries) * HEAD_K ** (-0.5)
    keys_now = rotate(keys_now)
    first_head = (lax.axis_index("z") * NC + lax.axis_index("c")) * heads
    head_level = (first_head + jnp.arange(heads)).astype(f32)
    retained = 1.0 - jnp.exp2(-5.0 - 16.0 * head_level / (HEADS - 1))
    new_state = (
        retained[None, :, None, None] * past_state
        + keys_now[:, :, :, None] * values_now[:, :, None, :]
    )
    retrieved = jnp.einsum("bhk,bhkv->bhv", queries, new_state)
    head_mean = jnp.mean(retrieved, axis=-1, keepdims=True)
    variance = jnp.mean(jnp.square(retrieved - head_mean), axis=-1, keepdims=True)
    normed = ((retrieved - head_mean) * lax.rsqrt(variance + EPS_GROUP)).reshape(rows, values_wide)
    mixed_heads = (jax.nn.silu(gate_now) * (normed * head_gain)).astype(bf16)
    return in_order(mixed_heads), new_state


def gained(gain, *weights):
    both = jnp.concatenate(weights, axis=1).astype(f32)
    return (both * gain[:, None]).astype(bf16)


def shards(
    tokens,
    past_state,
    first_gain,
    first_gate,
    first_up,
    first_down,
    mix_gain,
    query_weight,
    key_weight,
    value_weight,
    output_gate_weight,
    head_gain,
    out_weight,
    second_gain,
    second_gate,
    second_up,
    second_down,
):
    first_in = along_x_by_relay(gained(first_gain, first_gate), gained(first_gain, first_up))
    first_out = along_x(first_down)
    mix_own = gained(mix_gain, query_weight, key_weight, value_weight, output_gate_weight)
    mix = along_x(jnp.concatenate([mix_own, out_weight], axis=1))
    second_in = along_x(gained(second_gain, second_gate, second_up))
    second_out = along_x(second_down)

    own_columns = tokens.shape[1]
    sizes = (NX, NZ, NC)

    by_rows = by_distance(tokens.reshape(NY, NX, NC, -1, own_columns), "y")
    rows = NY * by_rows.shape[3]
    by_rows = jnp.transpose(by_rows, (1, 2, 4, 0, 3)).reshape(NX * NC, own_columns, rows)
    arrived = exchanged(by_rows, ("x", "c")).reshape(NX, NC * own_columns, rows)
    whole = for_each(by_distance(arrived, "x"), "z")
    mine = jnp.moveaxis(whole, 1, 0).reshape(-1, rows).T

    branch = branch_half_in_turn(first_inner(mine, first_in), first_out, 0.5)
    mine = next_input(branch, mine)

    x = both_halves(mine)
    inner, state_out = token_inner(x, mix, past_state, head_gain)
    branch = branch_half(inner, mix, 1.0)
    mine = next_input(branch, mine)

    x = both_halves(mine)
    branch = branch_half(channel_inner(x, times(x, second_in, second_in[0].shape[1])), second_out, 0.5)

    owner = jnp.arange(NZ) == lax.axis_index("z")
    chunks = jnp.moveaxis(mine.astype(f32).reshape(rows, NZ, LANES), 1, 0)
    branch = (branch + jnp.where(owner[:, None, None], chunks, 0.0)).astype(bf16)
    turned = by_distance(jnp.swapaxes(branch, 1, 2).reshape(NX, -1, rows), "x")
    arrived = exchanged(turned.reshape(-1, own_columns, rows), ("x", "z", "c"))
    arrived = arrived.reshape(*sizes, own_columns, rows).astype(f32).sum(axis=1).astype(bf16)
    arrived = arrived.reshape(NX, NC, own_columns, NY, -1)
    mixed = by_distance(jnp.transpose(arrived, (3, 0, 1, 4, 2)), "y").reshape(tokens.shape)
    return mixed, state_out


def solution(mesh):
    chips = Mesh(mesh.devices.reshape(NY, NX, NZ, NC), ("y", "x", "z", "c"))
    kv, tp = ("y", "x"), ("z", "c")
    in_specs = (
        P(None, kv + tp),
        P(kv, tp, None, None),
        P(kv),
        P(kv, tp),
        P(kv, tp),
        P(tp, kv),
        P(kv),
        P(kv, tp),
        P(kv, tp),
        P(kv, tp),
        P(kv, tp),
        P(tp),
        P(tp, kv),
        P(kv),
        P(kv, tp),
        P(kv, tp),
        P(tp, kv),
    )
    out_specs = (P(None, kv + tp), P(kv, tp, None, None))
    return jax.shard_map(shards, mesh=chips, in_specs=in_specs, out_specs=out_specs, check_vma=False)
```

```python
import jax
import jax.numpy as jnp
from jax import lax
from jax.experimental import pallas as pl
from jax.sharding import Mesh
from jax.sharding import PartitionSpec as P

D = 4096
HEADS = 32
HEAD_K = 64
HEAD_V = 128
POS = 16384
EPS_RMS = 1e-06
EPS_GROUP = 1e-05
ROPE_BASE = 10000.0
NY, NX, NZ, NC = 4, 4, 8, 2
LANES = 128


f32 = jnp.float32
bf16 = jnp.bfloat16


def swapped(value, axis, distance):
    return lax.ppermute(value, axis, [(i, i ^ distance) for i in range(lax.axis_size(axis))])


def exchanged(parts, axis):
    return lax.all_to_all(parts, axis, split_axis=0, concat_axis=0, tiled=True)


def for_each(value, axis):
    return exchanged(jnp.broadcast_to(value, (lax.axis_size(axis), *value.shape)), axis)


def along_x(block):
    one, three, two = (swapped(block, "x", d) for d in (1, 3, 2))
    return [block, one, two, three]


def along_x_by_relay(left, right):
    left_one = swapped(left, "x", 1)
    right_three = swapped(right, "x", 3)
    right_one = swapped(right, "x", 1)
    left_three = swapped(left, "x", 3)
    left_two = swapped(left_one, "x", 3)
    right_two = swapped(right_three, "x", 1)
    return [left, left_one, left_two, left_three], [right, right_one, right_two, right_three]


def by_distance(parts, axis):
    at = lax.axis_index(axis)
    picked = [lax.dynamic_slice_in_dim(parts, at ^ d, 1, axis=0) for d in range(parts.shape[0])]
    return jnp.concatenate(picked, axis=0)


def dot(a, b):
    return jnp.dot(a, b, preferred_element_type=f32)


def rotate(vectors):
    half_width = vectors.shape[-1] // 2
    frequency = ROPE_BASE ** (-jnp.arange(half_width, dtype=f32) / half_width)
    angles = POS * frequency
    cosine = jnp.cos(angles)
    sine_part = jnp.sin(angles)
    lower = vectors[..., :half_width]
    upper = vectors[..., half_width:]
    return jnp.concatenate(
        [lower * cosine - upper * sine_part, lower * sine_part + upper * cosine], axis=-1
    )


def inner_body(tiles, sides, width, mine, other, *refs):
    weights, targets = refs[:-NY], refs[-NY:]
    x = jnp.concatenate([mine[...], other[...]], axis=0)
    count = x.shape[0] // 2
    rows = count // NY
    depth = x.shape[1] // NX

    def put(at, value):
        for h in range(2):
            for d, target in enumerate(targets):
                part = value[h * count + d * rows : h * count + (d + 1) * rows]
                target[h * rows : (h + 1) * rows, at : at + value.shape[1]] = part.astype(
                    target.dtype
                )

    x_f = x.astype(f32)
    squares = jnp.sum(x_f * x_f, axis=1, keepdims=True)
    for side in range(sides):
        for start in range(0, width, 2 * LANES):
            size = min(2 * LANES, width - start)
            product = sum(
                dot(x[:, d * depth : (d + 1) * depth], w)
                for d, w in enumerate(tiles(weights, side, start, size))
            )
            spare = -size % LANES
            if spare:
                fill = jnp.broadcast_to(squares, (x.shape[0], spare))
                product = jnp.concatenate([product, fill], axis=1)
            put(side * (targets[0].shape[1] // 2) + start, product)
    if width % LANES == 0:
        put(sides * width, jnp.broadcast_to(squares, (x.shape[0], LANES)))


def apart(weights, side, start, size):
    return [w[:, start : start + size] for w in weights[side * NX : (side + 1) * NX]]


def packed(first_row, depth, blocks):
    def tiles(weights, side, start, size):
        at = first_row + (side * blocks + start // (2 * LANES)) * depth
        return [w[at : at + depth, :size] for w in weights]

    return tiles


def project(mine, weights, tiles, sides, width, total):
    other = swapped(mine, "c", 1)
    shape = (2 * mine.shape[0] // NY, total)
    own, *sent = pl.pallas_call(
        lambda *refs: inner_body(tiles, sides, width, *refs),
        out_shape=[jax.ShapeDtypeStruct(shape, t) for t in (f32, bf16, bf16, bf16)],
    )(mine, other, *weights)
    arrived = [swapped(sent[d - 1], "y", d) for d in (1, 3, 2)]
    return own + sum(a.astype(f32) for a in arrived)


def channel_inner(mine, weights, tiles, width):
    wide = width + -width % LANES
    with_squares = project(mine, weights, tiles, 2, width, 2 * wide)
    inverse_rms = lax.rsqrt(with_squares[:, width : width + 1] / D + EPS_RMS)
    gate = with_squares[:, :width] * inverse_rms
    up = with_squares[:, wide : wide + width] * inverse_rms
    return (jax.nn.silu(gate) * up).astype(bf16)


def branch_body(scale, p0, p1, p2, p3, w0, w1, w2, w3, mine, other):
    parts = [p[...] for p in (p0, p1, p2, p3)]
    count = p0.shape[0] // 2
    both = jnp.concatenate([p[:count] for p in parts] + [p[count:] for p in parts], axis=0)
    rows = NY * count
    for d, w in enumerate((w0, w1, w2, w3)):
        product = dot(both, w[...]) * scale
        for k in range(product.shape[1] // LANES):
            piece = product[:, k * LANES : (k + 1) * LANES]
            at = d * (product.shape[1] // LANES) + k
            mine[at] = piece[:rows].astype(mine.dtype)
            other[at] = piece[rows:].astype(other.dtype)


def branch_half(inner, weights, scale):
    one, three, two = (swapped(inner, "y", d) for d in (1, 3, 2))
    parts = (inner, one, two, three)
    depth, columns = inner.shape[1], weights[0].shape[1]
    width = NZ * LANES // NX
    shape = (NZ, NY * inner.shape[0] // 2, LANES)
    whole = pl.BlockSpec(inner.shape, lambda i: (0, 0))
    last = pl.BlockSpec((depth, width), lambda i: (0, columns // width - 1))
    out = pl.BlockSpec(shape, lambda i: (0, 0, 0))
    mine, other = pl.pallas_call(
        lambda *refs: branch_body(scale, *refs),
        grid=(1,),
        in_specs=[whole] * NY + [last] * NX,
        out_specs=[out, out],
        out_shape=[jax.ShapeDtypeStruct(shape, bf16)] * 2,
    )(*parts, *weights)
    arrived = swapped(other, "c", 1)
    return mine.astype(f32) + arrived.astype(f32)


def next_input(branch, mine):
    rows = mine.shape[0]
    own = lax.dynamic_slice(mine, (0, lax.axis_index("z") * LANES), (rows, LANES))
    arrived = exchanged(branch.astype(bf16), "z").astype(f32)
    piece = (arrived.sum(axis=0) + own.astype(f32)).astype(bf16)
    return jnp.moveaxis(for_each(piece, "z"), 0, 1).reshape(rows, NZ * LANES)


def in_order(rows):
    count = rows.shape[0] // 2
    return jnp.where(
        lax.axis_index("c") == 0, rows, jnp.concatenate([rows[count:], rows[:count]], axis=0)
    )


def token_inner(mine, weights, past_state, head_gain):
    rows, heads = past_state.shape[:2]
    keys_wide = heads * HEAD_K
    values_wide = heads * HEAD_V
    count = 2 * (keys_wide + values_wide)
    whole = project(mine, weights, apart, 1, count, count + LANES)
    inverse_rms = lax.rsqrt(whole[:, count : count + 1] / D + EPS_RMS)
    whole = in_order(whole[:, :count] * inverse_rms)
    queries = whole[:, :keys_wide].reshape(rows, heads, HEAD_K)
    keys_now = whole[:, keys_wide : 2 * keys_wide].reshape(rows, heads, HEAD_K)
    values_now = whole[:, 2 * keys_wide : 2 * keys_wide + values_wide].reshape(rows, heads, HEAD_V)
    gate_now = whole[:, 2 * keys_wide + values_wide :]
    queries = rotate(queries) * HEAD_K ** (-0.5)
    keys_now = rotate(keys_now)
    first_head = (lax.axis_index("z") * NC + lax.axis_index("c")) * heads
    head_level = (first_head + jnp.arange(heads)).astype(f32)
    retained = 1.0 - jnp.exp2(-5.0 - 16.0 * head_level / (HEADS - 1))
    new_state = (
        retained[None, :, None, None] * past_state
        + keys_now[:, :, :, None] * values_now[:, :, None, :]
    )
    retrieved = jnp.einsum("bhk,bhkv->bhv", queries, new_state)
    head_mean = jnp.mean(retrieved, axis=-1, keepdims=True)
    variance = jnp.mean(jnp.square(retrieved - head_mean), axis=-1, keepdims=True)
    normed = ((retrieved - head_mean) * lax.rsqrt(variance + EPS_GROUP)).reshape(rows, values_wide)
    mixed_heads = (jax.nn.silu(gate_now) * (normed * head_gain)).astype(bf16)
    return in_order(mixed_heads), new_state


def in_column_blocks(weights):
    size = 2 * LANES
    padded = jnp.pad(weights, ((0, 0), (0, -weights.shape[1] % size)))
    return jnp.split(padded, padded.shape[1] // size, axis=1)


def gained(gain, *weights):
    both = jnp.concatenate(weights, axis=1).astype(f32)
    return (both * gain[:, None]).astype(bf16)


def shards(
    tokens,
    past_state,
    first_gain,
    first_gate,
    first_up,
    first_down,
    mix_gain,
    query_weight,
    key_weight,
    value_weight,
    output_gate_weight,
    head_gain,
    out_weight,
    second_gain,
    second_gate,
    second_up,
    second_down,
):
    first_in = along_x_by_relay(gained(first_gain, first_gate), gained(first_gain, first_up))
    first_out = along_x(first_down)
    mix_own = gained(mix_gain, query_weight, key_weight, value_weight, output_gate_weight)
    mix = along_x(jnp.concatenate([mix_own, out_weight], axis=1))
    second = along_x(
        jnp.concatenate(
            [second_down]
            + in_column_blocks(gained(second_gain, second_gate))
            + in_column_blocks(gained(second_gain, second_up)),
            axis=0,
        ),
    )

    own_columns = tokens.shape[1]
    sizes = (NX, NZ, NC)

    by_rows = by_distance(tokens.reshape(NY, NX, NC, -1, own_columns), "y")
    rows = NY * by_rows.shape[3]
    by_rows = jnp.transpose(by_rows, (1, 2, 4, 0, 3)).reshape(NX * NC, own_columns, rows)
    arrived = exchanged(by_rows, ("x", "c")).reshape(NX, NC * own_columns, rows)
    whole = for_each(by_distance(arrived, "x"), "z")
    mine = jnp.moveaxis(whole, 1, 0).reshape(-1, rows).T

    width = first_gate.shape[1]
    inner = channel_inner(mine, first_in[0] + first_in[1], apart, width)
    branch = branch_half(inner, first_out, 0.5)
    mine = next_input(branch, mine)

    inner, state_out = token_inner(mine, mix, past_state, head_gain)
    branch = branch_half(inner, mix, 1.0)
    mine = next_input(branch, mine)

    depth = second_gate.shape[0]
    tiles = packed(width, depth, -(-width // (2 * LANES)))
    inner = channel_inner(mine, second, tiles, width)
    branch = branch_half(inner, second, 0.5)

    owner = jnp.arange(NZ) == lax.axis_index("z")
    chunks = jnp.moveaxis(mine.astype(f32).reshape(rows, NZ, LANES), 1, 0)
    branch = (branch + jnp.where(owner[:, None, None], chunks, 0.0)).astype(bf16)
    turned = by_distance(jnp.swapaxes(branch, 1, 2).reshape(NX, -1, rows), "x")
    arrived = exchanged(turned.reshape(-1, own_columns, rows), ("x", "z", "c"))
    arrived = arrived.reshape(*sizes, own_columns, rows).astype(f32).sum(axis=1).astype(bf16)
    arrived = arrived.reshape(NX, NC, own_columns, NY, -1)
    mixed = by_distance(jnp.transpose(arrived, (3, 0, 1, 4, 2)), "y").reshape(tokens.shape)
    return mixed, state_out


def solution(mesh):
    chips = Mesh(mesh.devices.reshape(NY, NX, NZ, NC), ("y", "x", "z", "c"))
    kv, tp = ("y", "x"), ("z", "c")
    in_specs = (
        P(None, kv + tp),
        P(kv, tp, None, None),
        P(kv),
        P(kv, tp),
        P(kv, tp),
        P(tp, kv),
        P(kv),
        P(kv, tp),
        P(kv, tp),
        P(kv, tp),
        P(kv, tp),
        P(tp),
        P(tp, kv),
        P(kv),
        P(kv, tp),
        P(kv, tp),
        P(tp, kv),
    )
    out_specs = (P(None, kv + tp), P(kv, tp, None, None))
    return jax.shard_map(shards, mesh=chips, in_specs=in_specs, out_specs=out_specs, check_vma=False)
```
